32 devices in a mesh: grp: 2 (over x), ep: 4 (over y, core), tp: 4 (over z).
Axes of the slice: x: 2, y: 2, z: 4, core: 2. Of those that a mesh axis runs over, the one named last changes fastest.
Arguments:
- pool_input: bfloat16 [8192, 1024], P(('grp', 'ep'), 'tp'), parts along dimension 0, may hold values from -6 to 6
- pool_map: bfloat16 [8, 128, 128], replicated, may hold values from -0.5 to 0.5
- pool_scale: float32 [1024], replicated, may hold values from 0.1 to 1.9
- out_weight: bfloat16 [1024, 2048], P(None, 'tp'), may hold values from -0.1875 to 0.1875
- expert_input: bfloat16 [4096, 2048], P(('grp', 'ep', 'tp')), parts along dimension 0, may hold values from -6 to 6
- norm_gain: float32 [2048], replicated, may hold values from 0.1 to 1.9
- routes: int32 [4096, 2], P(('grp', 'ep', 'tp')), parts along dimension 0, may hold values from 0 to 15, all different within a row; in each aligned block of 128 rows (0 to 127, 128 to 255, ...) at most 32 rows name the same one
- route_weight: float32 [4096, 2], P(('grp', 'ep', 'tp')), parts along dimension 0, may hold values from 0.2 to 1.5
- gate_weight: bfloat16 [16, 2048, 512], P(('ep', 'tp')), may hold values from -0.125 to 0.125
- up_weight: bfloat16 [16, 2048, 512], P(('ep', 'tp')), may hold values from -0.125 to 0.125
- down_weight: bfloat16 [16, 512, 2048], P(('ep', 'tp')), may hold values from -0.25 to 0.25
Outputs:
- pool_output: bfloat16 [8192, 2048], P(('grp', 'ep'), 'tp'), parts along dimension 0
- expert_output: bfloat16 [4096, 2048], P(('grp', 'ep', 'tp')), parts along dimension 0
The draws below stay inside these ranges and needn't reach their ends.
There are 2 independent parts, one for each index of `grp`. The reference program is written for one: setup_inputs(seed, part) draws one part's arguments, and reference() takes and returns one part's arrays. A program takes and returns all parts, laid end to end along the dimension named above; an argument that names none is the same for every part. Nothing has to cross between parts.
Inputs may be any that keep to these rules, and one draw needn't show every extreme that they name: `routes`: each row names 2 different experts. In the rows of one device no expert is named more than 32 times, and in every draw some device names some expert exactly 32 times.
All inputs are finite; a program needn't handle non-finite values.
Results may differ from the reference program's by a relative error of at most 0.007.
Values may be sent and summed in bfloat16 or wider, within the bound.
No kernel may reach another device: no remote copies, remote signals or barrier semaphores. Data moves between devices by JAX's collectives and lax.ppermute only.
A program may use at most 64 MiB of HBM per device.

```python
import math
import jax
import jax.numpy as jnp
import numpy as np
from jax import lax

D = 2048
D_EXPERT = 512
GROUP_DIM = 128
GROUPS = 8
TOP_K = 2
ROWS_B = 128
D_POOL = 1024
EXPERTS = 16
CAP = 32
TOKENS_A = 4096
TOKENS_B = 2048
N_EP = 4
N_TP = 4


def shard_levels(key, shape, split, low, top_value):
    loudness = 1.0
    for position, blocks in split:
        draws = jax.random.uniform(jax.random.fold_in(jax.random.fold_in(key, 6), position), (blocks,), jnp.float32, low / len(split), top_value / len(split))
        loudness = loudness * jnp.repeat(jnp.exp(draws), shape[position] // blocks).reshape((-1,) + (1,) * (len(shape) - 1 - position))
    return loudness


def routed_block(key, own, number, rows, amount, top, bound, skew):
    sequence = jax.random.permutation(key, amount)
    heavy_load, common = shares(amount, rows * top, bound, skew, True), shares(amount, rows * top, bound, skew, False)
    places = jnp.arange(amount)

    def named(tallies, turn):
        used = int((tallies > 0).sum())
        fixed = max(1, used // 4)
        moved = fixed + (places - fixed + turn * (used - fixed)) % max(1, amount - fixed)
        return jnp.zeros((amount,), jnp.int32).at[sequence[jnp.where(places < fixed, places, moved)]].set(jnp.asarray(tallies, jnp.int32))

    tallies = jnp.where(number % 4 == 0, named(heavy_load, number // 4), named(common, number - number // 4 - 1))
    mixed = jax.random.permutation(jax.random.fold_in(own, 3), amount)
    giver, receiver = mixed[0:amount // 2 * 2:2], mixed[1:amount // 2 * 2:2]
    margin = jnp.minimum(tallies[giver] - 1, bound - tallies[receiver]) // 2
    margin = jnp.where((giver == sequence[0]) | (receiver == sequence[0]) | (tallies[receiver] == 0), 0, jnp.maximum(margin, 0))
    moved = jax.random.randint(jax.random.fold_in(own, 4), (amount // 2,), 0, 1 << 20) % (margin + 1)
    tallies = tallies.at[giver].add(-moved).at[receiver].add(moved)
    labels = jnp.searchsorted(jnp.cumsum(tallies), jnp.arange(rows * top), side="right").astype(jnp.int32)
    grid = labels.reshape(top, rows).T
    grid = grid[jax.random.permutation(jax.random.fold_in(own, 1), rows)]
    turn = jax.random.randint(jax.random.fold_in(own, 2), (rows, 1), 0, top)
    return jnp.take_along_axis(grid, (jnp.arange(top)[None, :] + turn) % top, axis=1)


def shares(amount, total, limit, skew, full):
    weights = [(1 << 20) // math.isqrt(standing ** skew) + 1 for standing in range(1, amount + 1)]
    largest = limit if full else min(limit, max(-(-total // amount), total * weights[0] // sum(weights)))
    least = 1 if total - largest >= amount - 1 else 0
    given, spare = [largest] + [least] * (amount - 1), total - largest - least * (amount - 1)
    while spare > 0:
        candidates = [i for i in range(1, amount) if given[i] < largest] or [i for i in range(1, amount) if given[i] < limit]
        whole, remaining = sum([weights[i] for i in candidates]), spare
        for i in candidates:
            more = min(limit - given[i], max(1, remaining * weights[i] // whole), spare)
            given[i] = given[i] + more
            spare = spare - more
    return np.array(given)


def scatter_about(stream_key, shape, width, bound, pieces=(), held_as=jnp.bfloat16):
    values = jax.random.normal(stream_key, shape, jnp.float32) * width
    if len(pieces) > 0:
        values = shard_levels(stream_key, shape, pieces, -0.22, 0.18) * values
    return jnp.clip(values, min=-bound, max=bound).astype(held_as)


def setup_inputs(seed: int = 0, part: int = 0) -> dict:
    seeds = jax.random.split(jax.random.key(seed), 12)
    part_splits = jax.random.split(jax.random.fold_in(seeds[11], part), 12)
    pool_input = scatter_about(part_splits[0], (TOKENS_A, D_POOL), 1.0, 6.0, ((0, 4), (1, 4)))
    pool_map = scatter_about(seeds[1], (GROUPS, GROUP_DIM, GROUP_DIM), GROUP_DIM ** -0.5, 0.5)
    pool_scale = jnp.clip(1.0 + 0.18 * jax.random.normal(seeds[2], (D_POOL,), jnp.float32), 0.1, 1.9)
    out_weight = scatter_about(seeds[3], (D_POOL, D), D_POOL ** -0.5, 0.1875, ((1, 4),))
    expert_input = scatter_about(part_splits[4], (TOKENS_B, D), 1.0, 6.0, ((0, 16),))
    norm_gain = jnp.clip(1.0 + 0.18 * jax.random.normal(seeds[5], (D,), jnp.float32), 0.1, 1.9)
    routes_keys = jax.random.split(jax.random.fold_in(part_splits[6], 1), TOKENS_B // ROWS_B)
    routes_turns = jax.random.permutation(jax.random.fold_in(part_splits[6], 3), TOKENS_B // ROWS_B)
    routes = jax.vmap(lambda own, number: routed_block(jax.random.fold_in(part_splits[6], 2), own, number, ROWS_B, EXPERTS, TOP_K, CAP, 2))(routes_keys, routes_turns).reshape((TOKENS_B, TOP_K))
    route_weight = jnp.clip(0.2 + 1.3 * jax.random.uniform(part_splits[7], (TOKENS_B, TOP_K), jnp.float32) ** shard_levels(part_splits[7], (TOKENS_B, TOP_K), ((0, 16),), -0.2, 0.2), 0.2, 1.5)
    gate_weight = scatter_about(seeds[8], (EXPERTS, D, D_EXPERT), D ** -0.5, 0.125, ((0, 16),))
    up_weight = scatter_about(seeds[9], (EXPERTS, D, D_EXPERT), D ** -0.5, 0.125, ((0, 16),))
    down_weight = scatter_about(seeds[10], (EXPERTS, D_EXPERT, D), D_EXPERT ** -0.5, 0.25, ((0, 16),))
    return {"pool_input": pool_input, "pool_map": pool_map, "pool_scale": pool_scale, "out_weight": out_weight, "expert_input": expert_input, "norm_gain": norm_gain, "routes": routes, "route_weight": route_weight, "gate_weight": gate_weight, "up_weight": up_weight, "down_weight": down_weight}


epsilon = 1e-06

def pool_group(column_block, window):
    length = column_block.shape[0]
    running = jnp.cumsum(column_block, axis=0)
    earlier = jnp.pad(running, ((window, 0), (0, 0)))[:length]
    counted = jnp.minimum(jnp.arange(length) + 1, window).astype(jnp.float32)
    return (running - earlier) / counted[:, None] - column_block

def reference(pool_input, pool_map, pool_scale, out_weight, expert_input, norm_gain, routes, route_weight, gate_weight, up_weight, down_weight):
    widened = pool_input.astype(jnp.float32)
    mapped_parts = []
    for group_index in range(GROUPS):
        window = 2 ** (1 + group_index % 4)
        lower = group_index * GROUP_DIM
        columns = widened[:, lower:lower + GROUP_DIM]
        pooled = pool_group(columns, window).astype(jnp.bfloat16)
        mapped = jnp.dot(pooled, pool_map[group_index], preferred_element_type=jnp.float32)
        mapped = mapped * pool_scale[lower:lower + GROUP_DIM]
        mapped_parts.append(mapped.astype(jnp.bfloat16))
    mapped_all = jnp.concatenate(mapped_parts, axis=1)
    pool_output = jnp.dot(mapped_all, out_weight, preferred_element_type=jnp.float32).astype(jnp.bfloat16)
    widened_b = expert_input.astype(jnp.float32)
    normed = widened_b * lax.rsqrt(lax.optimization_barrier(jnp.mean(widened_b * widened_b, axis=1, keepdims=True)) + epsilon) * norm_gain
    normed = normed.astype(jnp.bfloat16)
    devices_all = N_EP * N_TP
    copies = ROWS_B * TOP_K
    flat_routes = routes.reshape(devices_all, copies).astype(jnp.int32)
    onehot = (flat_routes[:, :, None] == jnp.arange(EXPERTS, dtype=jnp.int32)[None, None, :]).astype(jnp.int32)
    before = jnp.cumsum(onehot, axis=1) - onehot
    slot_index = lax.optimization_barrier(jnp.sum(before * onehot, axis=2)).astype(jnp.int32)
    device_of = jnp.arange(devices_all, dtype=jnp.int32)[:, None]
    target = (flat_routes * (devices_all * CAP) + device_of * CAP + slot_index).astype(jnp.int32)
    token_of = (device_of * ROWS_B + jnp.arange(copies, dtype=jnp.int32)[None, :] // TOP_K).astype(jnp.int32)
    slot_count = EXPERTS * devices_all * CAP
    slot_table = jnp.full((slot_count,), TOKENS_B, jnp.int32).at[target.reshape(-1)].set(token_of.reshape(-1))
    slot_weight = jnp.zeros((slot_count,), jnp.float32).at[target.reshape(-1)].set(route_weight.astype(jnp.float32).reshape(-1))
    padded = jnp.concatenate([normed, jnp.zeros((1, D), jnp.bfloat16)], axis=0)

    def one_expert(accumulated, inputs):
        tokens_here, weights_here, gate_here, up_here, down_here = inputs
        rows_here = padded[tokens_here]
        gate_part = jnp.dot(rows_here, gate_here, preferred_element_type=jnp.float32)
        up_part = jnp.dot(rows_here, up_here, preferred_element_type=jnp.float32)
        hidden = (jax.nn.silu(gate_part) * up_part).astype(jnp.bfloat16)
        result = jnp.dot(hidden, down_here, preferred_element_type=jnp.float32).astype(jnp.bfloat16)
        accumulated = accumulated.at[tokens_here].add(weights_here[:, None] * result.astype(jnp.float32))
        return (accumulated, None)
    initial = jnp.zeros((TOKENS_B + 1, D), jnp.float32)
    accumulated, unused = lax.scan(one_expert, initial, (slot_table.reshape(EXPERTS, -1), slot_weight.reshape(EXPERTS, -1), gate_weight, up_weight, down_weight))
    expert_output = accumulated[:TOKENS_B].astype(jnp.bfloat16)
    return (pool_output, expert_output)
```

```python
import jax
import jax.numpy as jnp
from jax import lax
from jax.sharding import PartitionSpec as P

epsilon = 1e-06
halo_depth = 16
f32 = jnp.float32
bf16 = jnp.bfloat16


def moved(block, axis, by, keep):
    size = lax.axis_size(axis)
    pairs = [(i, i + by) for i in range(size) if 0 <= i + by < size and keep(i)]
    return lax.ppermute(block, axis, pairs)


def gather_line(block, axis):
    size = lax.axis_size(axis)
    from_left, from_right = [block], [block]
    for step in range(1, size):
        from_left.append(moved(from_left[-1], axis, 1, lambda i: i >= step - 1))
        from_right.append(moved(from_right[-1], axis, -1, lambda i: i <= size - step))
    blocks = [block]
    own = lax.axis_index(axis)
    for m in range(1, size):
        blocks.append(jnp.where(own + m < size, from_right[m], from_left[size - m]))
    return blocks, (from_left[-1], from_right[-1])


def scatter_line(partials, axis):
    size = lax.axis_size(axis)
    right, left = None, None
    for step in range(1, size):
        to_right, to_left = partials[size - step], partials[step]
        if step > 1:
            to_right, to_left = to_right + right.astype(f32), to_left + left.astype(f32)
        right = moved(to_right.astype(bf16), axis, 1, lambda i: i <= step - 1)
        left = moved(to_left.astype(bf16), axis, -1, lambda i: i >= size - step)
    total = partials[0]
    if size > 1:
        total = total + right.astype(f32) + left.astype(f32)
    return total


def expert_rows(received, gate_weight, up_weight, down_weight):
    shape_in = received.shape
    flat_rows = received.reshape(-1, shape_in[-1])
    gate_part = jnp.dot(flat_rows, gate_weight[0], preferred_element_type=f32)
    up_part = jnp.dot(flat_rows, up_weight[0], preferred_element_type=f32)
    hidden = (jax.nn.silu(gate_part) * up_part).astype(bf16)
    result = jnp.dot(hidden, down_weight[0], preferred_element_type=f32).astype(bf16)
    return result.reshape(shape_in)


def pool_mapped(pool_input, pool_map, pool_scale):
    row_count, width_local = pool_input.shape
    group_dim = pool_map.shape[1]
    groups_local = width_local // group_dim
    last_rows = pool_input[row_count - halo_depth :]
    earlier_rows = moved(last_rows, "ep", 1, lambda i: True)
    extended = jnp.concatenate([earlier_rows, pool_input], axis=0).astype(f32)
    first_group = lax.axis_index("tp") * groups_local
    group_ids = first_group + jnp.arange(width_local, dtype=jnp.int32) // group_dim
    window = jnp.left_shift(jnp.int32(2), group_ids % 4)
    summed = jnp.zeros((row_count, width_local), f32)
    for offset in range(halo_depth):
        shifted = extended[halo_depth - offset : halo_depth - offset + row_count]
        summed = summed + jnp.where(offset < window, shifted, 0.0)
    positions = lax.axis_index("ep") * row_count + jnp.arange(row_count, dtype=jnp.int32)
    counted = jnp.minimum(positions[:, None] + 1, window[None, :]).astype(f32)
    pooled = (summed / counted - extended[halo_depth:]).astype(bf16)
    maps_local = lax.dynamic_slice_in_dim(pool_map, first_group, groups_local, 0)
    scales_local = lax.dynamic_slice_in_dim(pool_scale, first_group * group_dim, width_local, 0)
    mapped = jnp.einsum(
        "rgc,gcd->rgd",
        pooled.reshape(row_count, groups_local, group_dim),
        maps_local,
        preferred_element_type=f32,
    )
    return (mapped.reshape(row_count, width_local) * scales_local).astype(bf16)


def pool_project(blocks, out_weight):
    size = len(blocks)
    depth = blocks[0].shape[1]
    own = lax.axis_index("tp")
    total = None
    for m in range(size):
        rows = lax.dynamic_slice_in_dim(out_weight, (own + m) % size * depth, depth, 0)
        product = jnp.dot(blocks[m], rows, preferred_element_type=f32)
        total = product if total is None else total + product
    return total.astype(bf16)


def on_device(
    pool_input,
    pool_map,
    pool_scale,
    out_weight,
    expert_input,
    norm_gain,
    routes,
    route_weight,
    gate_weight,
    up_weight,
    down_weight,
):
    row_count, model_width = expert_input.shape
    top_count = routes.shape[1]
    ep_count = lax.axis_size("ep")
    tp_count = lax.axis_size("tp")
    capacity = 2 * row_count * top_count // (ep_count * tp_count)
    own = lax.axis_index("tp")

    widened = expert_input.astype(f32)
    normed = (
        widened
        * lax.rsqrt(jnp.mean(widened * widened, axis=1, keepdims=True) + epsilon)
        * norm_gain
    ).astype(bf16)
    tokens, last_tokens = gather_line(normed, "tp")

    facts = jnp.concatenate([routes.astype(f32), route_weight], axis=1).T
    facts = lax.all_gather(facts, "tp", axis=0, tiled=False)
    facts = jnp.concatenate([facts, facts], axis=0)
    facts = lax.dynamic_slice_in_dim(facts, own, tp_count, 0)
    routes_all = facts[:, :top_count].astype(jnp.int32)
    weights_all = facts[:, top_count:]
    named = jnp.arange(ep_count, dtype=jnp.int32) * tp_count + own
    match = (routes_all[:, :, None, :] == named[None, None, :, None]).astype(f32)
    chosen = match.sum(axis=1)
    scale = (match * weights_all[:, :, None, :]).sum(axis=1)
    earlier = (
        jnp.arange(row_count, dtype=jnp.int32)[:, None]
        < jnp.arange(row_count, dtype=jnp.int32)[None, :]
    ).astype(bf16)
    rank = jnp.dot(
        chosen.reshape(-1, row_count).astype(bf16), earlier, preferred_element_type=f32
    ).reshape(tp_count, ep_count, row_count).astype(jnp.int32)
    slots = jnp.arange(capacity, dtype=jnp.int32)
    taken = (rank[:, :, None, :] == slots[None, None, :, None]) & (chosen[:, :, None, :] > 0)

    groups = [
        [m for m in range(tp_count) if m not in (1, tp_count - 1)],
        sorted({1, tp_count - 1} & set(range(1, tp_count))),
    ]
    partials = [None] * tp_count
    for group in groups:
        if not group:
            continue
        count = len(group)
        taken_here = jnp.stack([taken[m] for m in group], axis=1)
        scale_here = jnp.stack([scale[m] for m in group], axis=1)
        same = jnp.eye(count, dtype=bool)[None, :, None, :, None]
        select = (taken_here[:, :, :, None, :] & same).astype(bf16)
        rows = ep_count * count * capacity
        outgoing = jnp.dot(
            select.reshape(rows, count * row_count),
            jnp.concatenate([tokens[m] for m in group], axis=0),
            preferred_element_type=f32,
        ).astype(bf16)
        received = lax.all_to_all(
            outgoing.reshape(ep_count, count * capacity, model_width), "ep", 0, 0, tiled=True
        )
        results = expert_rows(received, gate_weight, up_weight, down_weight)
        returned = lax.all_to_all(results, "ep", 0, 0, tiled=True).reshape(rows, model_width)
        for place, m in enumerate(group):
            mine = taken_here & (jnp.arange(count) == place)[None, :, None, None]
            weighted = jnp.where(mine, scale_here[:, :, None, :], 0.0).reshape(rows, row_count).T
            upper = weighted.astype(bf16)
            lower = (weighted - upper.astype(f32)).astype(bf16)
            partials[m] = jnp.dot(upper, returned, preferred_element_type=f32) + jnp.dot(
                lower, returned, preferred_element_type=f32
            )

    mapped = pool_mapped(pool_input, pool_map, pool_scale)
    mapped, last_tokens = lax.optimization_barrier((mapped, last_tokens))
    pool_blocks, unused = gather_line(mapped, "tp")
    pool_output = pool_project(pool_blocks, out_weight)
    expert_output = scatter_line(partials, "tp").astype(bf16)
    return (pool_output, expert_output)


def solution(mesh):
    return jax.shard_map(
        on_device,
        mesh=mesh,
        in_specs=(
            P(("grp", "ep"), "tp"),
            P(),
            P(),
            P(None, "tp"),
            P(("grp", "ep", "tp"), None),
            P(),
            P(("grp", "ep", "tp"), None),
            P(("grp", "ep", "tp"), None),
            P(("ep", "tp"), None, None),
            P(("ep", "tp"), None, None),
            P(("ep", "tp"), None, None),
        ),
        out_specs=(P(("grp", "ep"), "tp"), P(("grp", "ep", "tp"), None)),
        check_vma=False,
    )
```

```python
import jax
import jax.numpy as jnp
from jax import lax
from jax.sharding import PartitionSpec as P

epsilon = 1e-06
halo_depth = 16
f32 = jnp.float32
bf16 = jnp.bfloat16


def moved(block, axis, by, keep):
    size = lax.axis_size(axis)
    pairs = [(i, i + by) for i in range(size) if 0 <= i + by < size and keep(i)]
    return lax.ppermute(block, axis, pairs)


def offset_blocks(block, from_left, from_right, axis):
    size = lax.axis_size(axis)
    own = lax.axis_index(axis)
    blocks = [block]
    for m in range(1, size):
        blocks.append(jnp.where(own + m < size, from_right[m], from_left[size - m]))
    return blocks


def gather_step(step, from_left, from_right, axis):
    size = lax.axis_size(axis)
    to_right, to_left = lax.optimization_barrier((from_left[-1], from_right[-1]))
    from_left.append(moved(to_right, axis, 1, lambda i: i >= step - 1))
    from_right.append(moved(to_left, axis, -1, lambda i: i <= size - step))


def after(value, *others):
    return lax.optimization_barrier((value,) + others)[0]


def expert_rows(received, gate_weight, up_weight, down_weight):
    shape_in = received.shape
    flat_rows = received.reshape(-1, shape_in[-1])
    gate_part = jnp.dot(flat_rows, gate_weight[0], preferred_element_type=f32)
    up_part = jnp.dot(flat_rows, up_weight[0], preferred_element_type=f32)
    hidden = (jax.nn.silu(gate_part) * up_part).astype(bf16)
    result = jnp.dot(hidden, down_weight[0], preferred_element_type=f32).astype(bf16)
    return result.reshape(shape_in)


def pool_mapped(pool_input, pool_map, pool_scale):
    row_count, width_local = pool_input.shape
    group_dim = pool_map.shape[1]
    groups_local = width_local // group_dim
    last_rows = pool_input[row_count - halo_depth :]
    earlier_rows = moved(last_rows, "ep", 1, lambda i: True)
    extended = jnp.concatenate([earlier_rows, pool_input], axis=0).astype(f32)
    first_group = lax.axis_index("tp") * groups_local
    group_ids = first_group + jnp.arange(width_local, dtype=jnp.int32) // group_dim
    window = jnp.left_shift(jnp.int32(2), group_ids % 4)
    summed = jnp.zeros((row_count, width_local), f32)
    for offset in range(halo_depth):
        shifted = extended[halo_depth - offset : halo_depth - offset + row_count]
        summed = summed + jnp.where(offset < window, shifted, 0.0)
    positions = lax.axis_index("ep") * row_count + jnp.arange(row_count, dtype=jnp.int32)
    counted = jnp.minimum(positions[:, None] + 1, window[None, :]).astype(f32)
    pooled = (summed / counted - extended[halo_depth:]).astype(bf16)
    maps_local = lax.dynamic_slice_in_dim(pool_map, first_group, groups_local, 0)
    scales_local = lax.dynamic_slice_in_dim(pool_scale, first_group * group_dim, width_local, 0)
    mapped = jnp.einsum(
        "rgc,gcd->rgd",
        pooled.reshape(row_count, groups_local, group_dim),
        maps_local,
        preferred_element_type=f32,
    )
    return (mapped.reshape(row_count, width_local) * scales_local).astype(bf16)


def pool_project(blocks, out_weight):
    size = len(blocks)
    depth = blocks[0].shape[1]
    own = lax.axis_index("tp")
    total = None
    for m in range(size):
        rows = lax.dynamic_slice_in_dim(out_weight, (own + m) % size * depth, depth, 0)
        product = jnp.dot(blocks[m], rows, preferred_element_type=f32)
        total = product if total is None else total + product
    return total.astype(bf16)


def on_device(
    pool_input,
    pool_map,
    pool_scale,
    out_weight,
    expert_input,
    norm_gain,
    routes,
    route_weight,
    gate_weight,
    up_weight,
    down_weight,
):
    row_count, model_width = expert_input.shape
    top_count = routes.shape[1]
    ep_count = lax.axis_size("ep")
    tp_count = lax.axis_size("tp")
    capacity = 2 * row_count * top_count // (ep_count * tp_count)
    experts = ep_count * tp_count
    parts = 2 if capacity % 2 == 0 else 1
    depth = capacity // parts

    widened = expert_input.astype(f32)
    normed = (
        widened
        * lax.rsqrt(jnp.mean(widened * widened, axis=1, keepdims=True) + epsilon)
        * norm_gain
    ).astype(bf16)

    named = jnp.arange(experts, dtype=jnp.int32)
    match = routes.T[:, None, :] == named[None, :, None]
    chosen = match.any(axis=0)
    scale = jnp.where(match, route_weight.T[:, None, :], 0.0).sum(axis=0)
    count = jnp.arange(row_count, dtype=jnp.int32)
    earlier = (count[:, None] < count[None, :]).astype(bf16)
    rank = jnp.dot(chosen.astype(bf16), earlier, preferred_element_type=f32).astype(jnp.int32)
    rank = jnp.where(chosen, rank, capacity)

    def taken(part):
        slots = part * depth + jnp.arange(depth, dtype=jnp.int32)
        return rank[:, None, :] == slots[None, :, None]

    def exchanged(rows):
        shape = rows.shape
        rows = rows.reshape(experts, depth, model_width)
        rows = lax.all_to_all(rows, ("ep", "tp"), split_axis=0, concat_axis=0, tiled=True)
        return rows.reshape(shape)

    received = []
    for part in range(parts):
        select = taken(part).astype(bf16).reshape(experts * depth, row_count)
        outgoing = jnp.dot(select, normed, preferred_element_type=f32).astype(bf16)
        received.append(exchanged(outgoing))

    mapped = pool_mapped(pool_input, pool_map, pool_scale)
    pool_left, pool_right = [mapped], [mapped]
    for step in range(1, tp_count):
        gather_step(step, pool_left, pool_right, "tp")

    total = None
    for part in range(parts):
        results = expert_rows(received[part], gate_weight, up_weight, down_weight)
        returned = exchanged(results)
        weighted = jnp.where(taken(part), scale[:, None, :], 0.0)
        weighted = weighted.reshape(experts * depth, row_count).T
        upper = weighted.astype(bf16)
        lower = (weighted - upper.astype(f32)).astype(bf16)
        product = jnp.dot(upper, returned, preferred_element_type=f32)
        product = product + jnp.dot(lower, returned, preferred_element_type=f32)
        total = product if total is None else total + product

    pool_blocks = offset_blocks(mapped, pool_left, pool_right, "tp")
    return (pool_project(pool_blocks, out_weight), total.astype(bf16))


def solution(mesh):
    return jax.shard_map(
        on_device,
        mesh=mesh,
        in_specs=(
            P(("grp", "ep"), "tp"),
            P(),
            P(),
            P(None, "tp"),
            P(("grp", "ep", "tp"), None),
            P(),
            P(("grp", "ep", "tp"), None),
            P(("grp", "ep", "tp"), None),
            P(("ep", "tp"), None, None),
            P(("ep", "tp"), None, None),
            P(("ep", "tp"), None, None),
        ),
        out_specs=(P(("grp", "ep"), "tp"), P(("grp", "ep", "tp"), None)),
        check_vma=False,
    )
```
